32 devices in a mesh: sp: 8 (over z, x), tp: 4 (over y, core).
Axes of the slice: x: 2, y: 2, z: 4, core: 2. Of those that a mesh axis runs over, the one named last changes fastest.
Arguments:
- residual: bfloat16 [4096, 2048], P(('sp', 'tp')), may hold values from -6 to 6
- queries: bfloat16 [4096, 1024], P('sp', 'tp'), may hold values from -6 to 6
- key_vectors: bfloat16 [4096, 1024], P('sp', 'tp'), may hold values from -6 to 6
- value_vectors: bfloat16 [4096, 1024], P('sp', 'tp'), may hold values from -6 to 6
- output_gate: bfloat16 [4096, 1024], P('sp', 'tp'), may hold values from -6 to 6
- input_gate: float32 [4096, 16], P('sp', 'tp'), may hold values from -4 to 250
- forget_gate: float32 [4096, 16], P('sp', 'tp'), may hold values from 0 to 20
- head_gain: float32 [16, 64], P('tp'), may hold values from 0.1 to 1.9
- output_weight: bfloat16 [1024, 2048], replicated, may hold values from -0.1875 to 0.1875
- norm_gain: float32 [2048], replicated, may hold values from 0.1 to 1.9
- route_experts: int32 [4096, 2], P('sp'), may hold values from 0 to 7, as said below
- group_weight: float32 [4096], P('sp'), may hold values from 0.25 to 1
- expert_scores: float32 [4096, 2], P('sp'), may hold values from -6 to 6
- gate_weight: bfloat16 [8, 2048, 1024], P('sp', None, 'tp'), may hold values from -0.125 to 0.125
- up_weight: bfloat16 [8, 2048, 1024], P('sp', None, 'tp'), may hold values from -0.125 to 0.125
- down_weight: bfloat16 [8, 1024, 2048], P('sp', 'tp'), may hold values from -0.1875 to 0.1875
Outputs:
- mixed_out: bfloat16 [4096, 2048], P(('sp', 'tp'))
The draws below stay inside these ranges and needn't reach their ends.
Inputs may be any that keep to these rules, and one draw needn't show every extreme that they name: `route_experts`: the two experts of a row differ and lie in the same group of 2 consecutive experts. In each aligned block of 128 rows no expert is named more than 64 times, and in every block some expert is named exactly 64 times.
All inputs are finite; a program needn't handle non-finite values.
Results may differ from the reference program's by a relative error of at most 0.012.
Values may be sent and summed in bfloat16 or wider, within the bound.
A program may use at most 128 MiB of HBM per device.

```python
import jax
import jax.numpy as jnp
from jax import lax

D = 2048
CELL_HEAD_COUNT = 16
HEAD = 64
MIX = 1024
FFE = 1024
GROUPS = 4
TOP = 2
BLOCK = 128
TOK_DEV = 128
SEQUENCE_TOKENS = 4096
EXPERTS = 8
CAP = 64
N_TP = 4


def draw_input_gate(key, part):
    base_value = jnp.clip(jax.random.normal(jax.random.fold_in(key, 11), (SEQUENCE_TOKENS, CELL_HEAD_COUNT), jnp.float32), -4.0, 4.0)
    return base_value


def draw_forget_gate(key, part):
    head_order = jax.random.permutation(jax.random.fold_in(key, 21), CELL_HEAD_COUNT)
    slow_count = CELL_HEAD_COUNT // 2
    sluggish_heads = head_order < slow_count
    step_rate = jnp.where(sluggish_heads, 0.6 / SEQUENCE_TOKENS, 1.0 / 40.0).astype(jnp.float32)
    device_span = SEQUENCE_TOKENS // EXPERTS
    factor = jnp.exp(jax.random.uniform(jax.random.fold_in(key, 22), (SEQUENCE_TOKENS // device_span, CELL_HEAD_COUNT), jnp.float32, -0.6931, 0.6931))
    factor = jnp.repeat(factor, device_span, axis=0)
    jitter = jnp.clip(0.7 * jax.random.normal(jax.random.fold_in(key, 23), (SEQUENCE_TOKENS, CELL_HEAD_COUNT), jnp.float32), -2.1, 2.1)
    gate_preactivation = -jnp.log(step_rate[None, :] * factor) + jitter
    surge_mask = (jax.random.uniform(jax.random.fold_in(key, 24), (SEQUENCE_TOKENS, CELL_HEAD_COUNT), jnp.float32) < 1.5 / SEQUENCE_TOKENS) & sluggish_heads[None, :]
    retained_fraction = 0.6 + 0.2 * jax.random.uniform(jax.random.fold_in(key, 25), (SEQUENCE_TOKENS, CELL_HEAD_COUNT), jnp.float32)
    return jnp.where(surge_mask, jnp.log(retained_fraction / (1.0 - retained_fraction)), gate_preactivation)


def draw_route_experts(key, part):
    block_total = SEQUENCE_TOKENS // TOK_DEV
    per_group = EXPERTS // GROUPS
    places = EXPERTS * CAP // 2
    position = jnp.arange(places, dtype=jnp.int32)
    group_of = position // (per_group * CAP // 2)
    inner_index = position % (per_group * CAP // 2)
    round_index = inner_index // per_group
    first_slot = inner_index % per_group
    second = (first_slot + 1 + round_index % (per_group - 1)) % per_group
    hot_expert = jax.random.randint(jax.random.fold_in(key, 31), (), 0, EXPERTS, dtype=jnp.int32)
    involved = (group_of == hot_expert // per_group) & ((first_slot == hot_expert % per_group) | (second == hot_expert % per_group))

    def one_block(block_key):
        rank_order = jax.random.permutation(jax.random.fold_in(block_key, 1), places).astype(jnp.int32)
        priority = rank_order + places * involved.astype(jnp.int32)
        _, chosen = lax.top_k(priority, TOK_DEV)
        chosen = chosen[jax.random.permutation(jax.random.fold_in(block_key, 2), TOK_DEV)]
        swap_order = jax.random.randint(jax.random.fold_in(block_key, 3), (TOK_DEV,), 0, 2, dtype=jnp.int32)
        expert_first = group_of[chosen] * per_group + first_slot[chosen]
        expert_second = group_of[chosen] * per_group + second[chosen]
        left_side = jnp.where(swap_order == 1, expert_second, expert_first)
        right_side = jnp.where(swap_order == 1, expert_first, expert_second)
        return jnp.stack([left_side, right_side], axis=1)
    block_keys = jax.random.split(jax.random.fold_in(key, 32), block_total)
    return jax.vmap(one_block)(block_keys).reshape(SEQUENCE_TOKENS, TOP).astype(jnp.int32)


def steps_of(key, extent, cuts, low, high):
    factor_of = 1.0
    for dim, blocks in cuts:
        steps = jax.random.uniform(jax.random.fold_in(jax.random.fold_in(key, 6), dim), (blocks,), jnp.float32, low / len(cuts), high / len(cuts))
        factor_of = factor_of * jnp.repeat(jnp.exp(steps), extent[dim] // blocks).reshape((-1,) + (1,) * (len(extent) - 1 - dim))
    return factor_of


def gaussian(rng, shape, width, bound, cuts=(), held_as=jnp.bfloat16):
    array = width * jax.random.normal(rng, shape, jnp.float32)
    if cuts:
        array = array * steps_of(rng, shape, cuts, -0.22, 0.18)
    return jnp.clip(array, -bound, bound).astype(held_as)


def setup_inputs(seed: int = 0) -> dict:
    streams_of = jax.random.split(jax.random.key(seed), 17)
    residual = gaussian(streams_of[0], (SEQUENCE_TOKENS, D), 1.0, 6.0, ((0, 32),))
    queries = gaussian(streams_of[1], (SEQUENCE_TOKENS, MIX), 1.0, 6.0, ((0, 8), (1, 4)))
    key_vectors = gaussian(streams_of[2], (SEQUENCE_TOKENS, MIX), 1.0, 6.0, ((0, 8), (1, 4)))
    value_vectors = gaussian(streams_of[3], (SEQUENCE_TOKENS, MIX), 1.0, 6.0, ((0, 8), (1, 4)))
    output_gate = gaussian(streams_of[4], (SEQUENCE_TOKENS, MIX), 1.0, 6.0, ((0, 8), (1, 4)))
    input_gate = draw_input_gate(jax.random.fold_in(streams_of[16], 71), 0)
    forget_gate = draw_forget_gate(jax.random.fold_in(streams_of[16], 71), 0)
    head_gain = jnp.clip(1.0 + 0.18 * jax.random.normal(streams_of[7], (CELL_HEAD_COUNT, HEAD), jnp.float32), 0.1, 1.9)
    output_weight = gaussian(streams_of[8], (MIX, D), MIX ** -0.5, 0.1875)
    norm_gain = jnp.clip(1.0 + 0.18 * jax.random.normal(streams_of[9], (D,), jnp.float32), 0.1, 1.9)
    route_experts = draw_route_experts(jax.random.fold_in(streams_of[16], 71), 0)
    group_weight = jnp.clip(0.25 + 0.75 * jax.random.uniform(streams_of[11], (SEQUENCE_TOKENS,), jnp.float32) ** steps_of(streams_of[11], (SEQUENCE_TOKENS,), ((0, 8),), -0.2, 0.2), 0.25, 1.0)
    expert_scores = gaussian(streams_of[12], (SEQUENCE_TOKENS, TOP), 1.5, 6.0, ((0, 8),), jnp.float32)
    gate_weight = gaussian(streams_of[13], (EXPERTS, D, FFE), D ** -0.5, 0.125, ((0, 8), (2, 4)))
    up_weight = gaussian(streams_of[14], (EXPERTS, D, FFE), D ** -0.5, 0.125, ((0, 8), (2, 4)))
    down_weight = gaussian(streams_of[15], (EXPERTS, FFE, D), FFE ** -0.5, 0.1875, ((0, 8), (1, 4)))
    return {"residual": residual, "queries": queries, "key_vectors": key_vectors, "value_vectors": value_vectors, "output_gate": output_gate, "input_gate": input_gate, "forget_gate": forget_gate, "head_gain": head_gain, "output_weight": output_weight, "norm_gain": norm_gain, "route_experts": route_experts, "group_weight": group_weight, "expert_scores": expert_scores, "gate_weight": gate_weight, "up_weight": up_weight, "down_weight": down_weight}


EPSILON = 1e-06
PRECISE = lax.Precision.HIGHEST

def block_step(carried, pieces):
    memory, stabilizer = carried
    query_block, key_block, value_block, decay_block, gate_block = pieces
    block_size = query_block.shape[0]
    causal_mask = jnp.tril(jnp.ones((block_size, block_size), dtype=bool))
    decay_rows = decay_block.T
    gate_rows = gate_block.T
    pair_log = decay_rows[:, :, None] - decay_rows[:, None, :] + gate_rows[:, None, :]
    pair_log = jnp.where(causal_mask[None], pair_log, -jnp.inf)
    carry_log = decay_rows + stabilizer[:, None]
    peak_level = jnp.maximum(carry_log, lax.optimization_barrier(jnp.max(pair_log, axis=-1)))
    within_weight = jnp.exp(pair_log - peak_level[:, :, None])
    carry_weight = jnp.exp(carry_log - peak_level)
    scores = jnp.einsum('thd,shd->hts', query_block, key_block, precision=PRECISE) * within_weight
    numerator = jnp.einsum('hts,shd->htd', scores, value_block, precision=PRECISE)
    numerator = numerator + carry_weight[:, :, None] * jnp.einsum('thd,hde->hte', query_block, memory, precision=PRECISE)
    outputs = jnp.transpose(numerator, (1, 0, 2))
    final_decay = decay_rows[:, -1]
    key_log = final_decay[:, None] - decay_rows + gate_rows
    new_level = jnp.maximum(final_decay + stabilizer, lax.optimization_barrier(jnp.max(key_log, axis=-1)))
    key_weight = jnp.exp(key_log - new_level[:, None])
    carry_fade = jnp.exp(final_decay + stabilizer - new_level)
    memory = carry_fade[:, None, None] * memory + jnp.einsum('hs,shd,she->hde', key_weight, key_block, value_block, precision=PRECISE)
    return ((memory, new_level), outputs)

def cell_outputs(query_part, key_part, value_part, input_gate, log_forget, initial):
    length, head_count, head_size = query_part.shape
    block_count = length // BLOCK
    cumulative = jnp.cumsum(log_forget.reshape(block_count, BLOCK, head_count), axis=1)
    shaped = (query_part.reshape(block_count, BLOCK, head_count, head_size), key_part.reshape(block_count, BLOCK, head_count, head_size), value_part.reshape(block_count, BLOCK, head_count, head_size), cumulative, input_gate.reshape(block_count, BLOCK, head_count))
    _, outputs = lax.scan(block_step, initial, shaped)
    return outputs.reshape(length, head_count, head_size)

def expert_sum(normed, route_experts, route_weight, gate_weight, up_weight, down_weight):
    flat_routes = route_experts.reshape(-1)
    flat_weights = jnp.concatenate([route_weight.reshape(-1), jnp.zeros((1,), jnp.float32)])
    padded = jnp.concatenate([normed, jnp.zeros((1, D), jnp.bfloat16)], axis=0)
    most_rows = CAP * (SEQUENCE_TOKENS // TOK_DEV)
    part_width = FFE // N_TP

    def one_expert(accumulated, expert):
        picked = jnp.nonzero(flat_routes == expert, size=most_rows, fill_value=flat_routes.shape[0])[0]
        token_of = picked // TOP
        chosen_rows = padded[token_of]
        gate_value = jnp.dot(chosen_rows, gate_weight[expert], preferred_element_type=jnp.float32)
        up_value = jnp.dot(chosen_rows, up_weight[expert], preferred_element_type=jnp.float32)
        hidden = (jax.nn.silu(gate_value) * up_value).astype(jnp.bfloat16)
        down_rows = down_weight[expert]
        summed = jnp.zeros((most_rows, D), jnp.float32)
        for quarter in range(N_TP):
            piece_out = jnp.dot(hidden[:, quarter * part_width:(quarter + 1) * part_width], down_rows[quarter * part_width:(quarter + 1) * part_width], preferred_element_type=jnp.float32).astype(jnp.bfloat16)
            summed = summed + lax.optimization_barrier(piece_out).astype(jnp.float32)
        rounded = lax.optimization_barrier(summed.astype(jnp.bfloat16))
        result = rounded.astype(jnp.float32) * flat_weights[picked][:, None]
        return (accumulated.at[token_of].add(result), None)
    accumulated = jnp.zeros((SEQUENCE_TOKENS + 1, D), jnp.float32)
    accumulated, _ = lax.scan(one_expert, accumulated, jnp.arange(EXPERTS, dtype=jnp.int32))
    return accumulated[:SEQUENCE_TOKENS]

def reference(residual, queries, key_vectors, value_vectors, output_gate, input_gate, forget_gate, head_gain, output_weight, norm_gain, route_experts, group_weight, expert_scores, gate_weight, up_weight, down_weight):
    query_part = queries.astype(jnp.float32).reshape(SEQUENCE_TOKENS, CELL_HEAD_COUNT, HEAD) * HEAD ** (-0.5)
    key_part = key_vectors.astype(jnp.float32).reshape(SEQUENCE_TOKENS, CELL_HEAD_COUNT, HEAD)
    value_part = value_vectors.astype(jnp.float32).reshape(SEQUENCE_TOKENS, CELL_HEAD_COUNT, HEAD)
    log_forget = jax.nn.log_sigmoid(forget_gate)
    initial = (jnp.zeros((CELL_HEAD_COUNT, HEAD, HEAD), jnp.float32), jnp.zeros((CELL_HEAD_COUNT,), jnp.float32))
    cell_out = cell_outputs(query_part, key_part, value_part, input_gate, log_forget, initial)
    normed_heads = cell_out * lax.rsqrt(lax.optimization_barrier(jnp.mean(cell_out * cell_out, axis=-1, keepdims=True)) + EPSILON) * head_gain
    mixed_rows = (jax.nn.sigmoid(output_gate.astype(jnp.float32)) * normed_heads.reshape(SEQUENCE_TOKENS, MIX)).astype(jnp.bfloat16)
    projected = jnp.dot(mixed_rows, output_weight, preferred_element_type=jnp.float32)
    stream = (residual.astype(jnp.float32) + projected).astype(jnp.bfloat16)
    stream_float = stream.astype(jnp.float32)
    normed = (stream_float * lax.rsqrt(lax.optimization_barrier(jnp.mean(stream_float * stream_float, axis=-1, keepdims=True)) + EPSILON) * norm_gain).astype(jnp.bfloat16)
    route_weight = group_weight[:, None] * jax.nn.softmax(expert_scores, axis=-1)
    expert_mix = expert_sum(normed, route_experts, route_weight, gate_weight, up_weight, down_weight)
    return (stream_float + expert_mix).astype(jnp.bfloat16)
```

```python
import functools

import jax
import jax.numpy as jnp
from jax import lax
from jax.experimental import pallas as pl
from jax.experimental.pallas import tpu as pltpu
from jax.sharding import PartitionSpec as P

TOP = 2
GROUPS = 4
BLOCK = 128

EPSILON = 1e-06
VERY_NEGATIVE = -1e30
PRECISE = lax.Precision.HIGHEST
MESH = pl.DeviceIdType.MESH
VMEM = pl.BlockSpec(memory_space=pltpu.VMEM)
ANY = pl.BlockSpec(memory_space=pl.ANY)


def remote(src, dst, send, recv, target):
    return pltpu.make_async_remote_copy(
        src_ref=src, dst_ref=dst, send_sem=send, recv_sem=recv, device_id=target, device_id_type=MESH
    )


def dot(a, b, **kw):
    return jnp.dot(a, b, preferred_element_type=jnp.float32, **kw)


def front_kernel(
    n_sp, n_tp, heads,
    q_ref, k_ref, v_ref, og_ref, ig_ref, fg_ref, gain_ref, ow_ref, res_ref, ngain_ref,
    stream_ref, normed_ref,
    num, run, msend, ssend, mrecv, srecv, mixed, arecv, wbuf,
    m_send, m_recv, s_send, s_recv, a_send, a_recv, w_sem,
):
    sp, tp = lax.axis_index("sp"), lax.axis_index("tp")
    length, width = q_ref.shape
    size = width // heads
    tokens = res_ref.shape[0]
    barrier = pltpu.get_barrier_semaphore()
    for off in range(1, n_sp):
        pl.semaphore_signal(
            barrier, inc=1, device_id={"sp": lax.rem(sp + off, n_sp)}, device_id_type=MESH
        )
    for off in range(1, n_tp):
        pl.semaphore_signal(
            barrier, inc=1, device_id={"tp": lax.rem(tp + off, n_tp)}, device_id_type=MESH
        )
    weight_copy = pltpu.make_async_copy(ow_ref, wbuf, w_sem)
    weight_copy.start()

    fg = fg_ref[...]
    log_forget = jnp.minimum(fg, 0.0) - jnp.log1p(jnp.exp(-jnp.abs(fg)))
    upper = (
        lax.broadcasted_iota(jnp.int32, (length, length), 0)
        <= lax.broadcasted_iota(jnp.int32, (length, length), 1)
    ).astype(jnp.float32)
    cum = dot(log_forget, upper, precision=PRECISE)
    level = ig_ref[...] - cum
    top = jnp.max(level, axis=1, keepdims=True)
    key_weight = jnp.exp(level - top)
    total = cum[:, length - 1 : length]
    key_t = k_ref[...].astype(jnp.float32).T
    for h in range(heads):
        cols = slice(h * size, (h + 1) * size)
        scaled = (key_t[cols] * key_weight[h : h + 1]).astype(jnp.bfloat16)
        msend[:, cols] = dot(scaled, v_ref[:, cols]).astype(jnp.bfloat16)
        ssend[0:1, cols] = jnp.broadcast_to(total[h : h + 1], (1, size))
        ssend[1:2, cols] = jnp.broadcast_to(total[h : h + 1] + top[h : h + 1], (1, size))

    def m_copy(slot, peer):
        return remote(msend, mrecv.at[slot], m_send.at[peer], m_recv.at[slot], {"sp": peer})

    def s_copy(slot, peer):
        return remote(ssend, srecv.at[slot], s_send.at[peer], s_recv.at[slot], {"sp": peer})

    pl.semaphore_wait(barrier, n_sp - 1 + n_tp - 1)
    for peer in range(n_sp - 1, 0, -1):

        @pl.when(peer > sp)
        def _():
            m_copy(sp, peer).start()
            s_copy(sp, peer).start()

    rows_n = BLOCK
    for b in range(length // rows_n):
        rows = slice(b * rows_n, (b + 1) * rows_n)
        upto = (b + 1) * rows_n
        row_at = lax.broadcasted_iota(jnp.int32, (rows_n, upto), 0) + b * rows_n
        causal = lax.broadcasted_iota(jnp.int32, (rows_n, upto), 1) <= row_at
        for h in range(heads):
            cols = slice(h * size, (h + 1) * size)
            line = level[h : h + 1, :upto]
            peak = jnp.max(jnp.where(causal, line, VERY_NEGATIVE), axis=1, keepdims=True)
            weight = jnp.where(causal, jnp.exp(line - peak), 0.0)
            scores = lax.dot_general(
                q_ref[rows, cols], k_ref[:upto, cols], (((1,), (1,)), ((), ())),
                preferred_element_type=jnp.float32,
            )
            num[rows, cols] = dot((scores * weight).astype(jnp.bfloat16), v_ref[:upto, cols])
            run[rows, cols] = jnp.broadcast_to(peak, (rows_n, size))

    for peer in range(n_sp):

        @pl.when(peer < sp)
        def _():
            m_copy(peer, peer).wait_recv()
            s_copy(peer, peer).wait_recv()

    def join(j, carried):
        state, start = carried
        stats = srecv[j]
        late_total, late = stats[0:1], stats[1:2]
        joined = jnp.maximum(late_total + start, late)
        state = state * jnp.exp(late_total + start - joined) + mrecv[j].astype(
            jnp.float32
        ) * jnp.exp(late - joined)
        return state, joined

    state, start = lax.fori_loop(
        0, sp, join, (jnp.zeros((size, width), jnp.float32), jnp.zeros((1, width), jnp.float32))
    )
    same = (
        lax.broadcasted_iota(jnp.int32, (width, width), 0) // size
        == lax.broadcasted_iota(jnp.int32, (width, width), 1) // size
    )
    spread = jnp.where(same, jnp.concatenate([state] * heads, axis=0), 0.0).astype(jnp.bfloat16)
    average = jnp.where(same, 1.0 / size, 0.0)
    for b in range(n_tp):
        rows = slice(b * tokens, (b + 1) * tokens)
        local = run[rows, :]
        peak = jnp.maximum(local, start)
        cell = (
            jnp.exp(local - peak) * num[rows, :] + jnp.exp(start - peak) * dot(q_ref[rows, :], spread)
        ) * size ** (-0.5)
        mean = dot(cell * cell, average, precision=PRECISE)
        normed = cell * lax.rsqrt(mean + EPSILON) * gain_ref[...]
        mixed[b] = (jax.nn.sigmoid(og_ref[rows, :].astype(jnp.float32)) * normed).astype(jnp.bfloat16)

    def a_copy(slot, peer):
        return remote(mixed.at[peer], arecv.at[slot], a_send.at[peer], a_recv.at[slot], {"tp": peer})

    for off in range(1, n_tp):
        a_copy(tp, lax.rem(tp + off, n_tp)).start()
    weight_copy.wait()

    def part(p):
        return wbuf[pl.ds(pl.multiple_of(p * width, width), width), :]

    acc = dot(mixed[tp], part(tp))
    for off in range(1, n_tp):
        p = lax.rem(tp + off, n_tp)
        a_copy(p, p).wait_recv()
        acc = acc + dot(arecv[p], part(p))
    stream = (res_ref[...].astype(jnp.float32) + acc).astype(jnp.bfloat16)
    stream_ref[...] = stream
    stream = stream.astype(jnp.float32)
    normed_ref[...] = (
        stream * lax.rsqrt(jnp.mean(stream * stream, axis=-1, keepdims=True) + EPSILON) * ngain_ref[...]
    ).astype(jnp.bfloat16)
    for peer in range(1, n_sp):

        @pl.when(peer > sp)
        def _():
            m_copy(sp, peer).wait_send()
            s_copy(sp, peer).wait_send()

    for off in range(1, n_tp):
        a_copy(tp, lax.rem(tp + off, n_tp)).wait_send()


def front(n_sp, n_tp, q, k, v, og, ig_t, fg_t, gain, ow, res, ngain):
    heads = ig_t.shape[0]
    length, width = q.shape
    size = width // heads
    tokens, model = res.shape
    f32, bf16 = jnp.float32, jnp.bfloat16
    dma = pltpu.SemaphoreType.DMA
    return pl.pallas_call(
        functools.partial(front_kernel, n_sp, n_tp, heads),
        out_shape=[jax.ShapeDtypeStruct((tokens, model), bf16)] * 2,
        in_specs=[VMEM] * 7 + [ANY] + [VMEM] * 2,
        out_specs=[VMEM] * 2,
        scratch_shapes=[
            pltpu.VMEM((length, width), f32),
            pltpu.VMEM((length, width), f32),
            pltpu.VMEM((size, width), bf16),
            pltpu.VMEM((8, width), f32),
            pltpu.VMEM((n_sp, size, width), bf16),
            pltpu.VMEM((n_sp, 8, width), f32),
            pltpu.VMEM((n_tp, tokens, width), bf16),
            pltpu.VMEM((n_tp, tokens, width), bf16),
            pltpu.VMEM(ow.shape, bf16),
            dma((n_sp,)), dma((n_sp,)), dma((n_sp,)), dma((n_sp,)), dma((n_tp,)), dma((n_tp,)), dma,
        ],
        compiler_params=pltpu.CompilerParams(
            collective_id=0, has_side_effects=True, vmem_limit_bytes=32 * 2**20
        ),
        cost_estimate=pl.CostEstimate(flops=4 * 10**9, bytes_accessed=8 * 2**20, transcendentals=0),
    )(q, k, v, og, ig_t, fg_t, gain, ow, res, ngain)


def plane_barrier(n_sp, z, x):
    barrier = pltpu.get_barrier_semaphore()
    groups = n_sp // TOP
    for off in range(1, groups):
        pl.semaphore_signal(
            barrier, inc=1, device_id={"sp": lax.rem(z + off, groups) * TOP + x}, device_id_type=MESH
        )
    pl.semaphore_signal(barrier, inc=1, device_id={"sp": z * TOP + 1 - x}, device_id_type=MESH)
    return lambda: pl.semaphore_wait(barrier, groups)


def send_kernel(
    n_sp, cap, normed_ref, group_ref, weight_ref, rows_ref, wts_ref,
    buf, wbuf, z_send, z_recv, x_send, x_recv, wz_send, wz_recv, wx_send, wx_recv,
):
    sp = lax.axis_index("sp")
    z, x = sp // TOP, lax.rem(sp, TOP)
    groups = n_sp // TOP
    arrive = plane_barrier(n_sp, z, x)
    tokens = normed_ref.shape[0]
    group = group_ref[...]
    hot = lax.broadcasted_iota(jnp.int32, (8, tokens), 0) == group
    before = (
        lax.broadcasted_iota(jnp.int32, (tokens, tokens), 0)
        < lax.broadcasted_iota(jnp.int32, (tokens, tokens), 1)
    )
    rank = dot(hot.astype(jnp.bfloat16), before.astype(jnp.bfloat16))
    slot = lax.broadcasted_iota(jnp.int32, (cap, tokens), 0).astype(jnp.float32)
    lane = lax.broadcasted_iota(jnp.int32, (128, tokens), 0).astype(jnp.float32)
    rows = normed_ref[...]
    for g in range(groups):
        here = group == g
        pick = jnp.where((slot == rank[g : g + 1]) & here, 1.0, 0.0).astype(jnp.bfloat16)
        wide = jnp.where((lane == rank[g : g + 1]) & here, 1.0, 0.0)
        buf[g] = dot(pick, rows).astype(jnp.bfloat16)
        wbuf[g] = lax.dot_general(
            weight_ref[...], wide, (((1,), (1,)), ((), ())),
            preferred_element_type=jnp.float32, precision=PRECISE,
        )
    arrive()
    other = {"sp": z * TOP + 1 - x}

    def z_copies(slot_z, peer_z):
        at, to = slot_z * TOP + x, {"sp": peer_z * TOP + x}
        return (
            remote(wbuf.at[peer_z], wts_ref.at[at], wz_send.at[peer_z], wz_recv.at[slot_z], to),
            remote(buf.at[peer_z], rows_ref.at[at], z_send.at[peer_z], z_recv.at[slot_z], to),
        )

    def x_own():
        return (
            remote(wbuf.at[z], wts_ref.at[sp], wx_send.at[z], wx_recv.at[z], other),
            remote(buf.at[z], rows_ref.at[sp], x_send.at[z], x_recv.at[z], other),
        )

    def x_copies(slot_z, side):
        at = slot_z * TOP + side
        return (
            remote(wts_ref.at[at], wts_ref.at[at], wx_send.at[slot_z], wx_recv.at[slot_z], other),
            remote(rows_ref.at[at], rows_ref.at[at], x_send.at[slot_z], x_recv.at[slot_z], other),
        )

    far = [lax.rem(z + off, groups) for off in range(1, groups)]
    for peer in far:
        for copy in z_copies(z, peer):
            copy.start()
    for copy in x_own():
        copy.start()
    rows_ref[sp] = buf[z]
    wts_ref[sp] = wbuf[z]
    for peer in far[::-1]:
        for copy in z_copies(peer, peer):
            copy.wait_recv()
        for copy in x_copies(peer, x):
            copy.start()
    for copy in x_copies(z, 1 - x):
        copy.wait_recv()
    for peer in far[::-1]:
        for copy in x_copies(peer, 1 - x):
            copy.wait_recv()
    for peer in far:
        for copy in z_copies(z, peer):
            copy.wait_send()
        for copy in x_copies(peer, x):
            copy.wait_send()
    for copy in x_own():
        copy.wait_send()


def send_rows_pair(n_sp, cap, normed, group, weight):
    groups = n_sp // TOP
    model = normed.shape[1]
    bf16, f32 = jnp.bfloat16, jnp.float32
    dma = pltpu.SemaphoreType.DMA
    return pl.pallas_call(
        functools.partial(send_kernel, n_sp, cap),
        out_shape=[
            jax.ShapeDtypeStruct((n_sp, cap, model), bf16),
            jax.ShapeDtypeStruct((n_sp, 8, 128), f32),
        ],
        in_specs=[VMEM] * 3,
        out_specs=[VMEM] * 2,
        scratch_shapes=[pltpu.VMEM((groups, cap, model), bf16), pltpu.VMEM((groups, 8, 128), f32)]
        + [dma((groups,))] * 8,
        compiler_params=pltpu.CompilerParams(
            collective_id=1, has_side_effects=True, vmem_limit_bytes=32 * 2**20
        ),
        cost_estimate=pl.CostEstimate(flops=10**9, bytes_accessed=64 * 2**20, transcendentals=0),
    )(normed, group, weight)


def back_kernel(
    n_sp, cap, out_ref, wts_ref, group_ref, stream_ref, final_ref,
    xsend, xrecv, zsend, zrecv, x_send, x_recv, z_send, z_recv,
):
    sp = lax.axis_index("sp")
    z, x = sp // TOP, lax.rem(sp, TOP)
    groups = n_sp // TOP
    arrive = plane_barrier(n_sp, z, x)
    tokens = stream_ref.shape[0]
    other = {"sp": z * TOP + 1 - x}
    diagonal = lax.broadcasted_iota(jnp.int32, (cap, cap), 0) == lax.broadcasted_iota(
        jnp.int32, (cap, cap), 1
    )

    def weighted(at):
        table = wts_ref[at]
        line = jnp.where(x == 0, table[0:1, :cap], table[1:2, :cap])
        column = jnp.sum(jnp.where(diagonal, line, 0.0), axis=1, keepdims=True)
        return column * out_ref[at].astype(jnp.float32)

    order = [lax.rem(z + off, groups) for off in (list(range(1, groups)) + [0])]

    def x_copy(at):
        return remote(xsend.at[at], xrecv.at[at], x_send.at[at], x_recv.at[at], other)

    def z_copy(slot_z, peer_z):
        to = {"sp": peer_z * TOP + x}
        return remote(zsend.at[peer_z], zrecv.at[slot_z], z_send.at[peer_z], z_recv.at[slot_z], to)

    for i, at in enumerate(order):
        xsend[at] = weighted(at * TOP + 1 - x).astype(jnp.bfloat16)
        if i == 0:
            arrive()
        x_copy(at).start()
    for i, at in enumerate(order):
        mine = weighted(at * TOP + x)
        x_copy(at).wait_recv()
        summed = (mine + xrecv[at].astype(jnp.float32)).astype(jnp.bfloat16)
        if i < groups - 1:
            zsend[at] = summed
            z_copy(z, at).start()
        else:
            zrecv[z] = summed
    group = group_ref[...]
    hot = lax.broadcasted_iota(jnp.int32, (tokens, 128), 1) == group
    before = (
        lax.broadcasted_iota(jnp.int32, (tokens, tokens), 1)
        < lax.broadcasted_iota(jnp.int32, (tokens, tokens), 0)
    )
    rank = dot(before.astype(jnp.bfloat16), hot.astype(jnp.bfloat16))
    own_rank = jnp.sum(jnp.where(hot, rank, 0.0), axis=1, keepdims=True)
    slot = lax.broadcasted_iota(jnp.int32, (tokens, cap), 1).astype(jnp.float32)
    fits = slot == own_rank
    acc = stream_ref[...].astype(jnp.float32)
    for at in order[-1:] + order[:-1][::-1]:
        if at is not order[-1]:
            z_copy(at, at).wait_recv()
        pick = jnp.where(fits & (group == at), 1.0, 0.0).astype(jnp.bfloat16)
        acc = acc + dot(pick, zrecv[at])
    final_ref[...] = acc.astype(jnp.bfloat16)
    for at in order:
        x_copy(at).wait_send()
    for at in order[:-1]:
        z_copy(z, at).wait_send()


def back_rows_pair(n_sp, cap, out, wts, group, stream):
    groups = n_sp // TOP
    model = stream.shape[1]
    dma = pltpu.SemaphoreType.DMA
    return pl.pallas_call(
        functools.partial(back_kernel, n_sp, cap),
        out_shape=jax.ShapeDtypeStruct(stream.shape, jnp.bfloat16),
        in_specs=[VMEM] * 4,
        out_specs=VMEM,
        scratch_shapes=[pltpu.VMEM((groups, cap, model), jnp.bfloat16)] * 4 + [dma((groups,))] * 4,
        compiler_params=pltpu.CompilerParams(
            collective_id=2, has_side_effects=True, vmem_limit_bytes=32 * 2**20
        ),
        cost_estimate=pl.CostEstimate(flops=10**9, bytes_accessed=64 * 2**20, transcendentals=0),
    )(out, wts, group, stream)


def weight_parts(own, axis, count):
    parts = [own]
    for k in range(1, count):
        low = k & -k
        parts.append(lax.ppermute(parts[k ^ low], axis, [(i, i ^ low) for i in range(count)]))
    return parts


def expert_parts(rows, gates, ups, downs):
    total = None
    for gate, up, down in zip(gates, ups, downs):
        hidden = (jax.nn.silu(dot(rows, gate[0])) * dot(rows, up[0])).astype(jnp.bfloat16)
        term = dot(hidden, down[0])
        total = term if total is None else total + term
    return total.astype(jnp.bfloat16)


def slot_within(flat_routes, expert_total):
    onehot = (flat_routes[:, None] == jnp.arange(expert_total, dtype=jnp.int32)[None, :]).astype(
        jnp.int32
    )
    before = jnp.cumsum(onehot, axis=0) - onehot
    return jnp.sum(before * onehot, axis=1)


def fill_slots(source_rows, places, slot_total):
    assign = jnp.arange(places.shape[0], dtype=jnp.int32) // TOP
    owner_index = jnp.full((slot_total,), source_rows.shape[0], jnp.int32).at[places].set(assign)
    padded = jnp.concatenate(
        [source_rows, jnp.zeros((1, source_rows.shape[1]), source_rows.dtype)], axis=0
    )
    return padded[owner_index]


def shards(
    residual, queries, key_vectors, value_vectors, output_gate, input_gate, forget_gate, head_gain,
    output_weight, norm_gain, route_experts, group_weight, expert_scores, gate_weight, up_weight,
    down_weight,
):
    token_count, model_width = residual.shape
    tp = lax.axis_index("tp")
    n_sp, n_tp = lax.axis_size("sp"), lax.axis_size("tp")
    gates = weight_parts(gate_weight, "tp", n_tp)
    ups = weight_parts(up_weight, "tp", n_tp)
    downs = weight_parts(down_weight, "tp", n_tp)
    stream, normed = front(
        n_sp, n_tp, queries, key_vectors, value_vectors, output_gate, input_gate.T, forget_gate.T,
        head_gain.reshape(1, -1), output_weight, residual, norm_gain.reshape(1, -1),
    )
    capacity = 2 * TOP * token_count // n_sp
    own_routes = lax.dynamic_slice_in_dim(route_experts, tp * token_count, token_count, 0)
    own_group = lax.dynamic_slice_in_dim(group_weight, tp * token_count, token_count, 0)
    own_scores = lax.dynamic_slice_in_dim(expert_scores, tp * token_count, token_count, 0)
    route_weight = own_group[:, None] * jax.nn.softmax(own_scores, axis=-1)
    if n_sp == GROUPS * TOP and token_count == 128:
        group = own_routes[:, 0] // TOP
        first = (own_routes[:, 0] % TOP) == 0
        weights = jnp.stack(
            [
                jnp.where(first, route_weight[:, 0], route_weight[:, 1]),
                jnp.where(first, route_weight[:, 1], route_weight[:, 0]),
            ]
        )
        weights = jnp.pad(weights, ((0, 8 - TOP), (0, 0)))
        rows, wts = send_rows_pair(n_sp, capacity, normed, group[None, :], weights)
        out = expert_parts(rows.reshape(n_sp * capacity, model_width), gates, ups, downs)
        return back_rows_pair(
            n_sp, capacity, out.reshape(n_sp, capacity, model_width), wts, group[:, None], stream
        )
    flat = own_routes.reshape(-1)
    places = flat * capacity + slot_within(flat, n_sp)
    send_rows = fill_slots(normed, places, n_sp * capacity)
    arrived = lax.all_to_all(
        send_rows.reshape(n_sp, capacity, model_width), "sp", split_axis=0, concat_axis=0, tiled=True
    )
    returned = expert_parts(arrived.reshape(n_sp * capacity, model_width), gates, ups, downs)
    answers = lax.all_to_all(
        returned.reshape(n_sp, capacity, model_width), "sp", split_axis=0, concat_axis=0, tiled=True
    )
    picked = (
        answers.reshape(n_sp * capacity, model_width)[places]
        .astype(jnp.float32)
        .reshape(token_count, TOP, model_width)
    )
    expert_mix = jnp.sum(picked * route_weight[:, :, None], axis=1)
    return (stream.astype(jnp.float32) + expert_mix).astype(jnp.bfloat16)


def solution(mesh):
    return jax.shard_map(
        shards,
        mesh=mesh,
        in_specs=(
            P(("sp", "tp"), None),
            P("sp", "tp"),
            P("sp", "tp"),
            P("sp", "tp"),
            P("sp", "tp"),
            P("sp", "tp"),
            P("sp", "tp"),
            P("tp", None),
            P(),
            P(),
            P("sp", None),
            P("sp"),
            P("sp", None),
            P("sp", None, "tp"),
            P("sp", None, "tp"),
            P("sp", "tp", None),
        ),
        out_specs=P(("sp", "tp"), None),
        check_vma=False,
    )
```

```python
import functools

import jax
import jax.numpy as jnp
from jax import lax
from jax.experimental import pallas as pl
from jax.experimental.pallas import tpu as pltpu
from jax.sharding import PartitionSpec as P

TOP = 2
GROUPS = 4
BLOCK = 128

EPSILON = 1e-06
VERY_NEGATIVE = -1e30
PRECISE = lax.Precision.HIGHEST
MESH = pl.DeviceIdType.MESH
VMEM = pl.BlockSpec(memory_space=pltpu.VMEM)
ANY = pl.BlockSpec(memory_space=pl.ANY)


def remote(src, dst, send, recv, target):
    return pltpu.make_async_remote_copy(
        src_ref=src, dst_ref=dst, send_sem=send, recv_sem=recv, device_id=target, device_id_type=MESH
    )


def dot(a, b, **kw):
    return jnp.dot(a, b, preferred_element_type=jnp.float32, **kw)


def nothing():
    return None


NO_HOOKS = {name: nothing for name in ("load", "entered", "keys", "queries", "exchanged")}


def front_kernel(
    n_sp, n_tp, heads, hooks,
    q_ref, k_ref, v_ref, og_ref, ig_ref, fg_ref, gain_ref, ow_ref, res_ref, ngain_ref,
    stream_ref, normed_ref,
    num, run, msend, ssend, mrecv, srecv, mixed, arecv, wbuf,
    m_send, m_recv, s_send, s_recv, a_send, a_recv, w_sem,
):
    sp, tp = lax.axis_index("sp"), lax.axis_index("tp")
    length, width = q_ref.shape
    size = width // heads
    tokens = res_ref.shape[0]
    barrier = pltpu.get_barrier_semaphore()
    for off in range(1, n_sp):
        pl.semaphore_signal(
            barrier, inc=1, device_id={"sp": lax.rem(sp + off, n_sp)}, device_id_type=MESH
        )
    for off in range(1, n_tp):
        pl.semaphore_signal(
            barrier, inc=1, device_id={"tp": lax.rem(tp + off, n_tp)}, device_id_type=MESH
        )
    weight_copy = pltpu.make_async_copy(ow_ref, wbuf, w_sem)
    hooks["load"]()
    weight_copy.start()

    fg = fg_ref[...]
    log_forget = jnp.minimum(fg, 0.0) - jnp.log1p(jnp.exp(-jnp.abs(fg)))
    upper = (
        lax.broadcasted_iota(jnp.int32, (length, length), 0)
        <= lax.broadcasted_iota(jnp.int32, (length, length), 1)
    ).astype(jnp.float32)
    cum = dot(log_forget, upper, precision=PRECISE)
    level = ig_ref[...] - cum
    top = jnp.max(level, axis=1, keepdims=True)
    key_weight = jnp.exp(level - top)
    total = cum[:, length - 1 : length]
    hooks["keys"]()
    key_t = k_ref[...].astype(jnp.float32).T
    for h in range(heads):
        cols = slice(h * size, (h + 1) * size)
        scaled = (key_t[cols] * key_weight[h : h + 1]).astype(jnp.bfloat16)
        msend[:, cols] = dot(scaled, v_ref[:, cols]).astype(jnp.bfloat16)
        ssend[0:1, cols] = jnp.broadcast_to(total[h : h + 1], (1, size))
        ssend[1:2, cols] = jnp.broadcast_to(total[h : h + 1] + top[h : h + 1], (1, size))

    def m_copy(slot, peer):
        return remote(msend, mrecv.at[slot], m_send.at[peer], m_recv.at[slot], {"sp": peer})

    def s_copy(slot, peer):
        return remote(ssend, srecv.at[slot], s_send.at[peer], s_recv.at[slot], {"sp": peer})

    pl.semaphore_wait(barrier, n_sp - 1 + n_tp - 1)
    hooks["entered"]()
    for peer in range(n_sp - 1, 0, -1):

        @pl.when(peer > sp)
        def _():
            m_copy(sp, peer).start()
            s_copy(sp, peer).start()

    hooks["queries"]()
    rows_n = BLOCK
    for b in range(length // rows_n):
        rows = slice(b * rows_n, (b + 1) * rows_n)
        upto = (b + 1) * rows_n
        row_at = lax.broadcasted_iota(jnp.int32, (rows_n, upto), 0) + b * rows_n
        causal = lax.broadcasted_iota(jnp.int32, (rows_n, upto), 1) <= row_at
        for h in range(heads):
            cols = slice(h * size, (h + 1) * size)
            line = level[h : h + 1, :upto]
            peak = jnp.max(jnp.where(causal, line, VERY_NEGATIVE), axis=1, keepdims=True)
            weight = jnp.where(causal, jnp.exp(line - peak), 0.0)
            scores = lax.dot_general(
                q_ref[rows, cols], k_ref[:upto, cols], (((1,), (1,)), ((), ())),
                preferred_element_type=jnp.float32,
            )
            num[rows, cols] = dot((scores * weight).astype(jnp.bfloat16), v_ref[:upto, cols])
            run[rows, cols] = jnp.broadcast_to(peak, (rows_n, size))

    for peer in range(n_sp):

        @pl.when(peer < sp)
        def _():
            m_copy(peer, peer).wait_recv()
            s_copy(peer, peer).wait_recv()

    def join(j, carried):
        state, start = carried
        stats = srecv[j]
        late_total, late = stats[0:1], stats[1:2]
        joined = jnp.maximum(late_total + start, late)
        state = state * jnp.exp(late_total + start - joined) + mrecv[j].astype(
            jnp.float32
        ) * jnp.exp(late - joined)
        return state, joined

    state, start = lax.fori_loop(
        0, sp, join, (jnp.zeros((size, width), jnp.float32), jnp.zeros((1, width), jnp.float32))
    )
    same = (
        lax.broadcasted_iota(jnp.int32, (width, width), 0) // size
        == lax.broadcasted_iota(jnp.int32, (width, width), 1) // size
    )
    spread = jnp.where(same, jnp.concatenate([state] * heads, axis=0), 0.0).astype(jnp.bfloat16)
    average = jnp.where(same, 1.0 / size, 0.0)
    for b in range(n_tp):
        rows = slice(b * tokens, (b + 1) * tokens)
        local = run[rows, :]
        peak = jnp.maximum(local, start)
        cell = (
            jnp.exp(local - peak) * num[rows, :] + jnp.exp(start - peak) * dot(q_ref[rows, :], spread)
        ) * size ** (-0.5)
        mean = dot(cell * cell, average, precision=PRECISE)
        normed = cell * lax.rsqrt(mean + EPSILON) * gain_ref[...]
        mixed[b] = (jax.nn.sigmoid(og_ref[rows, :].astype(jnp.float32)) * normed).astype(jnp.bfloat16)

    def a_copy(slot, peer):
        return remote(mixed.at[peer], arecv.at[slot], a_send.at[peer], a_recv.at[slot], {"tp": peer})

    for off in range(1, n_tp):
        a_copy(tp, lax.rem(tp + off, n_tp)).start()
    hooks["exchanged"]()
    weight_copy.wait()

    def part(p):
        return wbuf[pl.ds(pl.multiple_of(p * width, width), width), :]

    acc = dot(mixed[tp], part(tp))
    for off in range(1, n_tp):
        p = lax.rem(tp + off, n_tp)
        a_copy(p, p).wait_recv()
        acc = acc + dot(arecv[p], part(p))
    stream = (res_ref[...].astype(jnp.float32) + acc).astype(jnp.bfloat16)
    stream_ref[...] = stream
    stream = stream.astype(jnp.float32)
    normed_ref[...] = (
        stream * lax.rsqrt(jnp.mean(stream * stream, axis=-1, keepdims=True) + EPSILON) * ngain_ref[...]
    ).astype(jnp.bfloat16)
    for peer in range(1, n_sp):

        @pl.when(peer > sp)
        def _():
            m_copy(sp, peer).wait_send()
            s_copy(sp, peer).wait_send()

    for off in range(1, n_tp):
        a_copy(tp, lax.rem(tp + off, n_tp)).wait_send()


def front(n_sp, n_tp, q, k, v, og, ig_t, fg_t, gain, ow, res, ngain):
    heads = ig_t.shape[0]
    length, width = q.shape
    size = width // heads
    tokens, model = res.shape
    f32, bf16 = jnp.float32, jnp.bfloat16
    dma = pltpu.SemaphoreType.DMA
    return pl.pallas_call(
        functools.partial(front_kernel, n_sp, n_tp, heads, NO_HOOKS),
        out_shape=[jax.ShapeDtypeStruct((tokens, model), bf16)] * 2,
        in_specs=[VMEM] * 7 + [ANY] + [VMEM] * 2,
        out_specs=[VMEM] * 2,
        scratch_shapes=[
            pltpu.VMEM((length, width), f32),
            pltpu.VMEM((length, width), f32),
            pltpu.VMEM((size, width), bf16),
            pltpu.VMEM((8, width), f32),
            pltpu.VMEM((n_sp, size, width), bf16),
            pltpu.VMEM((n_sp, 8, width), f32),
            pltpu.VMEM((n_tp, tokens, width), bf16),
            pltpu.VMEM((n_tp, tokens, width), bf16),
            pltpu.VMEM(ow.shape, bf16),
            dma((n_sp,)), dma((n_sp,)), dma((n_sp,)), dma((n_sp,)), dma((n_tp,)), dma((n_tp,)), dma,
        ],
        compiler_params=pltpu.CompilerParams(
            collective_id=0, has_side_effects=True, vmem_limit_bytes=32 * 2**20
        ),
        cost_estimate=pl.CostEstimate(flops=4 * 10**9, bytes_accessed=8 * 2**20, transcendentals=0),
    )(q, k, v, og, ig_t, fg_t, gain, ow, res, ngain)


def whole_kernel(
    n_sp, n_tp, heads, cap,
    q_ref, k_ref, v_ref, og_ref, ig_ref, fg_ref, gain_ref, ow_ref, res_ref, ngain_ref,
    route_ref, share_ref, score_ref, gate_ref, up_ref, down_ref,
    final_ref,
    q_in, k_in, v_in, og_in, res_in, stream_ref, normed_ref,
    num, run, msend, ssend, mrecv, srecv, mixed, arecv, wbuf,
    gates, ups, downs, buf, tbuf, rows_ref, wts_ref, acc, xsend, xrecv, zsend, zrecv,
    m_send, m_recv, s_send, s_recv, a_send, a_recv, w_sem,
    in_sem, own_sem, c_send, c_recv, y_send, y_recv, f_send, f_recv,
    z_send, z_recv, x_send, x_recv, wz_send, wz_recv, wx_send, wx_recv,
    bx_send, bx_recv, bz_send, bz_recv,
):
    sp, tp = lax.axis_index("sp"), lax.axis_index("tp")
    z, x = sp // TOP, lax.rem(sp, TOP)
    groups = n_sp // TOP
    tokens = res_ref.shape[0]
    near = {"tp": tp + 1 - 2 * lax.rem(tp, 2)}
    across = {"tp": lax.rem(tp + n_tp // 2, n_tp)}
    other = {"sp": z * TOP + 1 - x}
    sources, held = (gate_ref, up_ref, down_ref), (gates, ups, downs)

    pairs = ((k_ref, k_in), (v_ref, v_in), (q_ref, q_in), (og_ref, og_in), (res_ref, res_in))
    loads = [pltpu.make_async_copy(src, dst, in_sem.at[i]) for i, (src, dst) in enumerate(pairs)]
    own = [pltpu.make_async_copy(sources[i], held[i].at[0], own_sem.at[i]) for i in range(3)]
    beside = [remote(sources[i], held[i].at[1], c_send.at[i], c_recv.at[i], near) for i in range(3)]
    over = [remote(sources[i], held[i].at[2], y_send.at[i], y_recv.at[i], across) for i in range(3)]
    onward = [remote(held[i].at[2], held[i].at[3], f_send.at[i], f_recv.at[i], near) for i in range(3)]

    def load():
        for copy in loads:
            copy.start()

    def entered():
        over[0].start()

    def keys():
        loads[0].wait()
        loads[1].wait()

    def queries():
        for copy in loads[2:]:
            copy.wait()
        for copy in beside + own:
            copy.start()

    def exchanged():
        over[1].start()
        over[2].start()

    hooks = {
        "load": load, "entered": entered, "keys": keys, "queries": queries, "exchanged": exchanged,
    }
    front_kernel(
        n_sp, n_tp, heads, hooks,
        q_in, k_in, v_in, og_in, ig_ref, fg_ref, gain_ref, ow_ref, res_in, ngain_ref,
        stream_ref, normed_ref,
        num, run, msend, ssend, mrecv, srecv, mixed, arecv, wbuf,
        m_send, m_recv, s_send, s_recv, a_send, a_recv, w_sem,
    )

    mine = pl.ds(pl.multiple_of(tp * tokens, tokens), tokens)
    first_route = route_ref[:, mine].astype(jnp.float32)[0:1]
    group = jnp.floor(first_route * (1.0 / TOP))
    even = (first_route - TOP * group) < 0.5
    score = score_ref[:, mine]
    power = jnp.exp(score - jnp.max(score, axis=0, keepdims=True))
    route_weight = share_ref[:, mine] * (power / jnp.sum(power, axis=0, keepdims=True))
    lead, rest = route_weight[0:1], route_weight[1:2]
    table = jnp.concatenate(
        [jnp.where(even, lead, rest), jnp.where(even, rest, lead), jnp.zeros((6, tokens), jnp.float32)],
        axis=0,
    )
    hot = lax.broadcasted_iota(jnp.int32, (8, tokens), 0).astype(jnp.float32) == group
    at_row = lax.broadcasted_iota(jnp.int32, (tokens, tokens), 0)
    at_lane = lax.broadcasted_iota(jnp.int32, (tokens, tokens), 1)
    rank = dot(
        jnp.where(hot, 1.0, 0.0).astype(jnp.bfloat16),
        jnp.where(at_row < at_lane, 1.0, 0.0).astype(jnp.bfloat16),
    )
    slot = lax.broadcasted_iota(jnp.int32, (cap, tokens), 0).astype(jnp.float32)
    lane = lax.broadcasted_iota(jnp.int32, (128, tokens), 0).astype(jnp.float32)
    for g in range(groups):
        here = group == float(g)
        pick = jnp.where((slot == rank[g : g + 1]) & here, 1.0, 0.0).astype(jnp.bfloat16)
        wide = jnp.where((lane == rank[g : g + 1]) & here, 1.0, 0.0)
        buf[g] = dot(pick, normed_ref[...]).astype(jnp.bfloat16)
        tbuf[g] = lax.dot_general(
            table, wide, (((1,), (1,)), ((), ())),
            preferred_element_type=jnp.float32, precision=PRECISE,
        )

    def z_copies(slot_z, peer_z):
        to = {"sp": peer_z * TOP + x}
        return (
            remote(tbuf.at[peer_z], wts_ref.at[x, slot_z], wz_send.at[peer_z], wz_recv.at[slot_z], to),
            remote(buf.at[peer_z], rows_ref.at[x, slot_z], z_send.at[peer_z], z_recv.at[slot_z], to),
        )

    def x_own():
        return (
            remote(tbuf.at[z], wts_ref.at[x, z], wx_send.at[z], wx_recv.at[z], other),
            remote(buf.at[z], rows_ref.at[x, z], x_send.at[z], x_recv.at[z], other),
        )

    def x_copies(slot_z, side):
        t, r = wts_ref.at[side, slot_z], rows_ref.at[side, slot_z]
        return (
            remote(t, t, wx_send.at[slot_z], wx_recv.at[slot_z], other),
            remote(r, r, x_send.at[slot_z], x_recv.at[slot_z], other),
        )

    far = [lax.rem(z + off, groups) for off in range(1, groups)]
    for peer in far:
        for copy in z_copies(z, peer):
            copy.start()
    for copy in x_own():
        copy.start()
    rows_ref[x, z] = buf[z]
    wts_ref[x, z] = tbuf[z]
    for i in range(3):
        own[i].wait()
        beside[i].wait()
    over[0].wait()
    onward[0].start()
    for peer in far[::-1]:
        for copy in z_copies(peer, peer):
            copy.wait_recv()
        for copy in x_copies(peer, x):
            copy.start()
    for peer in [z] + far[::-1]:
        for copy in x_copies(peer, 1 - x):
            copy.wait_recv()

    model = res_ref.shape[1]

    def quarter(k, side):
        block = rows_ref[side].reshape(groups * cap, model)
        hidden = (jax.nn.silu(dot(block, gates[k])) * dot(block, ups[k])).astype(jnp.bfloat16)
        term = dot(hidden, downs[k])
        if k == 0:
            acc[side] = term
        else:
            acc[side] += term

    for k in range(2):

        @pl.loop(0, 2)
        def _(side):
            quarter(k, side)

    for i in range(1, 3):
        over[i].wait()
        onward[i].start()

    @pl.loop(0, 2)
    def _(side):
        quarter(2, side)

    for i in range(3):
        onward[i].wait()

    diagonal = lax.broadcasted_iota(jnp.int32, (cap, cap), 0) == lax.broadcasted_iota(
        jnp.int32, (cap, cap), 1
    )

    def weighted(side, at):
        lines = wts_ref[side, at]
        line = jnp.where(x == 0, lines[0:1, :cap], lines[1:2, :cap])
        column = jnp.sum(jnp.where(diagonal, line, 0.0), axis=1, keepdims=True)
        return column * acc[side, pl.ds(pl.multiple_of(at * cap, cap), cap), :]

    order = far + [z]

    def x_copy(at):
        return remote(xsend.at[at], xrecv.at[at], bx_send.at[at], bx_recv.at[at], other)

    def z_copy(slot_z, peer_z):
        to = {"sp": peer_z * TOP + x}
        return remote(zsend.at[peer_z], zrecv.at[slot_z], bz_send.at[peer_z], bz_recv.at[slot_z], to)

    quarter(3, 1 - x)
    for at in order:
        xsend[at] = weighted(1 - x, at).astype(jnp.bfloat16)
        x_copy(at).start()
    quarter(3, x)
    for i, at in enumerate(order):
        kept = weighted(x, at)
        x_copy(at).wait_recv()
        summed = (kept + xrecv[at].astype(jnp.float32)).astype(jnp.bfloat16)
        if i < groups - 1:
            zsend[at] = summed
            z_copy(z, at).start()
        else:
            zrecv[z] = summed

    def turned(line):
        return jnp.sum(jnp.where(at_row == at_lane, line, 0.0), axis=1, keepdims=True)

    own_rank = turned(jnp.sum(jnp.where(hot, rank, 0.0), axis=0, keepdims=True))
    own_group = turned(group)
    fits = lax.broadcasted_iota(jnp.int32, (tokens, cap), 1).astype(jnp.float32) == own_rank
    total = stream_ref[...].astype(jnp.float32)
    for i, at in enumerate([z] + far[::-1]):
        if i:
            z_copy(at, at).wait_recv()
        level = at.astype(jnp.float32)
        pick = jnp.where(fits & (own_group == level), 1.0, 0.0).astype(jnp.bfloat16)
        total = total + dot(pick, zrecv[at])
    final_ref[...] = total.astype(jnp.bfloat16)
    for peer in far:
        for copy in z_copies(z, peer):
            copy.wait_send()
        for copy in x_copies(peer, x):
            copy.wait_send()
        z_copy(z, peer).wait_send()
    for copy in x_own():
        copy.wait_send()
    for at in order:
        x_copy(at).wait_send()


def whole(
    n_sp, n_tp, cap, q, k, v, og, ig_t, fg_t, gain, ow, res, ngain, route_t, share, score_t,
    gate, up, down,
):
    heads = ig_t.shape[0]
    length, width = q.shape
    size = width // heads
    tokens, model = res.shape
    groups = n_sp // TOP
    f32, bf16 = jnp.float32, jnp.bfloat16
    dma = pltpu.SemaphoreType.DMA
    vm = pltpu.VMEM
    return pl.pallas_call(
        functools.partial(whole_kernel, n_sp, n_tp, heads, cap),
        out_shape=jax.ShapeDtypeStruct((tokens, model), bf16),
        in_specs=[ANY] * 4 + [VMEM] * 3 + [ANY] * 2 + [VMEM] * 4 + [ANY] * 3,
        out_specs=VMEM,
        scratch_shapes=[vm((length, width), bf16)] * 4
        + [vm((tokens, model), bf16)] * 3
        + [
            vm((length, width), f32),
            vm((length, width), f32),
            vm((size, width), bf16),
            vm((8, width), f32),
            vm((n_sp, size, width), bf16),
            vm((n_sp, 8, width), f32),
            vm((n_tp, tokens, width), bf16),
            vm((n_tp, tokens, width), bf16),
            vm(ow.shape, bf16),
            vm((n_tp,) + gate.shape, bf16),
            vm((n_tp,) + up.shape, bf16),
            vm((n_tp,) + down.shape, bf16),
            vm((groups, cap, model), bf16),
            vm((groups, 8, 128), f32),
            vm((TOP, groups, cap, model), bf16),
            vm((TOP, groups, 8, 128), f32),
            vm((TOP, groups * cap, model), f32),
        ]
        + [vm((groups, cap, model), bf16)] * 4
        + [dma((n_sp,))] * 4
        + [dma((n_tp,))] * 2
        + [dma, dma((5,))]
        + [dma((3,))] * 7
        + [dma((groups,))] * 12,
        compiler_params=pltpu.CompilerParams(
            collective_id=1, has_side_effects=True, vmem_limit_bytes=60 * 2**20
        ),
    )(q, k, v, og, ig_t, fg_t, gain, ow, res, ngain, route_t, share, score_t, gate, up, down)


def weight_parts(own, axis, count):
    parts = [own]
    for k in range(1, count):
        low = k & -k
        parts.append(lax.ppermute(parts[k ^ low], axis, [(i, i ^ low) for i in range(count)]))
    return parts


def expert_parts(rows, gates, ups, downs):
    total = None
    for gate, up, down in zip(gates, ups, downs):
        hidden = (jax.nn.silu(dot(rows, gate[0])) * dot(rows, up[0])).astype(jnp.bfloat16)
        term = dot(hidden, down[0])
        total = term if total is None else total + term
    return total.astype(jnp.bfloat16)


def slot_within(flat_routes, expert_total):
    onehot = (flat_routes[:, None] == jnp.arange(expert_total, dtype=jnp.int32)[None, :]).astype(
        jnp.int32
    )
    before = jnp.cumsum(onehot, axis=0) - onehot
    return jnp.sum(before * onehot, axis=1)


def fill_slots(source_rows, places, slot_total):
    assign = jnp.arange(places.shape[0], dtype=jnp.int32) // TOP
    owner_index = jnp.full((slot_total,), source_rows.shape[0], jnp.int32).at[places].set(assign)
    padded = jnp.concatenate(
        [source_rows, jnp.zeros((1, source_rows.shape[1]), source_rows.dtype)], axis=0
    )
    return padded[owner_index]


def shards(
    residual, queries, key_vectors, value_vectors, output_gate, input_gate, forget_gate, head_gain,
    output_weight, norm_gain, route_experts, group_weight, expert_scores, gate_weight, up_weight,
    down_weight,
):
    token_count, model_width = residual.shape
    tp = lax.axis_index("tp")
    n_sp, n_tp = lax.axis_size("sp"), lax.axis_size("tp")
    capacity = 2 * TOP * token_count // n_sp
    if n_sp == GROUPS * TOP and n_tp == 4 and token_count == 128:
        return whole(
            n_sp, n_tp, capacity, queries, key_vectors, value_vectors, output_gate, input_gate.T,
            forget_gate.T, head_gain.reshape(1, -1), output_weight, residual,
            norm_gain.reshape(1, -1), route_experts.T, group_weight.reshape(1, -1),
            expert_scores.T, gate_weight[0], up_weight[0], down_weight[0],
        )
    own_routes = lax.dynamic_slice_in_dim(route_experts, tp * token_count, token_count, 0)
    own_group = lax.dynamic_slice_in_dim(group_weight, tp * token_count, token_count, 0)
    own_scores = lax.dynamic_slice_in_dim(expert_scores, tp * token_count, token_count, 0)
    route_weight = own_group[:, None] * jax.nn.softmax(own_scores, axis=-1)
    gates = weight_parts(gate_weight, "tp", n_tp)
    ups = weight_parts(up_weight, "tp", n_tp)
    downs = weight_parts(down_weight, "tp", n_tp)
    stream, normed = front(
        n_sp, n_tp, queries, key_vectors, value_vectors, output_gate, input_gate.T, forget_gate.T,
        head_gain.reshape(1, -1), output_weight, residual, norm_gain.reshape(1, -1),
    )
    flat = own_routes.reshape(-1)
    places = flat * capacity + slot_within(flat, n_sp)
    send_rows = fill_slots(normed, places, n_sp * capacity)
    arrived = lax.all_to_all(
        send_rows.reshape(n_sp, capacity, model_width), "sp", split_axis=0, concat_axis=0, tiled=True
    )
    returned = expert_parts(arrived.reshape(n_sp * capacity, model_width), gates, ups, downs)
    answers = lax.all_to_all(
        returned.reshape(n_sp, capacity, model_width), "sp", split_axis=0, concat_axis=0, tiled=True
    )
    picked = (
        answers.reshape(n_sp * capacity, model_width)[places]
        .astype(jnp.float32)
        .reshape(token_count, TOP, model_width)
    )
    expert_mix = jnp.sum(picked * route_weight[:, :, None], axis=1)
    return (stream.astype(jnp.float32) + expert_mix).astype(jnp.bfloat16)


def solution(mesh):
    return jax.shard_map(
        shards,
        mesh=mesh,
        in_specs=(
            P(("sp", "tp"), None),
            P("sp", "tp"),
            P("sp", "tp"),
            P("sp", "tp"),
            P("sp", "tp"),
            P("sp", "tp"),
            P("sp", "tp"),
            P("tp", None),
            P(),
            P(),
            P("sp", None),
            P("sp"),
            P("sp", None),
            P("sp", None, "tp"),
            P("sp", None, "tp"),
            P("sp", "tp", None),
        ),
        out_specs=P(("sp", "tp"), None),
        check_vma=False,
    )
```

```python
import functools

import jax
import jax.numpy as jnp
from jax import lax
from jax.experimental import pallas as pl
from jax.experimental.pallas import tpu as pltpu
from jax.sharding import PartitionSpec as P

TOP = 2
GROUPS = 4
BLOCK = 128
CHUNKS = 4

EPSILON = 1e-06
VERY_NEGATIVE = -1e30
PRECISE = lax.Precision.HIGHEST
MESH = pl.DeviceIdType.MESH
VMEM = pl.BlockSpec(memory_space=pltpu.VMEM)
ANY = pl.BlockSpec(memory_space=pl.ANY)


def remote(src, dst, send, recv, target):
    return pltpu.make_async_remote_copy(
        src_ref=src, dst_ref=dst, send_sem=send, recv_sem=recv, device_id=target, device_id_type=MESH
    )


def dot(a, b, **kw):
    return jnp.dot(a, b, preferred_element_type=jnp.float32, **kw)


def nothing():
    return None


NO_HOOKS = {name: nothing for name in ("load", "entered", "keys", "queries", "exchanged")}


def front_kernel(
    n_sp, n_tp, heads, hooks,
    q_ref, k_ref, v_ref, og_ref, ig_ref, fg_ref, gain_ref, ow_ref, res_ref, ngain_ref,
    stream_ref, normed_ref,
    num, run, msend, ssend, mrecv, srecv, mixed, arecv, wbuf,
    m_send, m_recv, s_send, s_recv, a_send, a_recv, w_sem,
):
    sp, tp = lax.axis_index("sp"), lax.axis_index("tp")
    length, width = q_ref.shape
    size = width // heads
    tokens = res_ref.shape[0]
    barrier = pltpu.get_barrier_semaphore()
    for off in range(1, n_sp):
        pl.semaphore_signal(
            barrier, inc=1, device_id={"sp": lax.rem(sp + off, n_sp)}, device_id_type=MESH
        )
    for off in range(1, n_tp):
        pl.semaphore_signal(
            barrier, inc=1, device_id={"tp": lax.rem(tp + off, n_tp)}, device_id_type=MESH
        )
    weight_copy = pltpu.make_async_copy(ow_ref, wbuf, w_sem)
    hooks["load"]()
    weight_copy.start()

    fg = fg_ref[...]
    log_forget = jnp.minimum(fg, 0.0) - jnp.log1p(jnp.exp(-jnp.abs(fg)))
    upper = (
        lax.broadcasted_iota(jnp.int32, (length, length), 0)
        <= lax.broadcasted_iota(jnp.int32, (length, length), 1)
    ).astype(jnp.float32)
    cum = dot(log_forget, upper, precision=PRECISE)
    level = ig_ref[...] - cum
    top = jnp.max(level, axis=1, keepdims=True)
    key_weight = jnp.exp(level - top)
    total = cum[:, length - 1 : length]
    hooks["keys"]()
    key_t = k_ref[...].astype(jnp.float32).T
    for h in range(heads):
        cols = slice(h * size, (h + 1) * size)
        scaled = (key_t[cols] * key_weight[h : h + 1]).astype(jnp.bfloat16)
        msend[:, cols] = dot(scaled, v_ref[:, cols]).astype(jnp.bfloat16)
        ssend[0:1, cols] = jnp.broadcast_to(total[h : h + 1], (1, size))
        ssend[1:2, cols] = jnp.broadcast_to(total[h : h + 1] + top[h : h + 1], (1, size))

    def m_copy(slot, peer):
        return remote(msend, mrecv.at[slot], m_send.at[peer], m_recv.at[slot], {"sp": peer})

    def s_copy(slot, peer):
        return remote(ssend, srecv.at[slot], s_send.at[peer], s_recv.at[slot], {"sp": peer})

    pl.semaphore_wait(barrier, n_sp - 1 + n_tp - 1)
    hooks["entered"]()
    for peer in range(n_sp - 1, 0, -1):

        @pl.when(peer > sp)
        def _():
            m_copy(sp, peer).start()
            s_copy(sp, peer).start()

    hooks["queries"]()
    rows_n = BLOCK
    for b in range(length // rows_n):
        rows = slice(b * rows_n, (b + 1) * rows_n)
        upto = (b + 1) * rows_n
        row_at = lax.broadcasted_iota(jnp.int32, (rows_n, upto), 0) + b * rows_n
        causal = lax.broadcasted_iota(jnp.int32, (rows_n, upto), 1) <= row_at
        for h in range(heads):
            cols = slice(h * size, (h + 1) * size)
            line = level[h : h + 1, :upto]
            peak = jnp.max(jnp.where(causal, line, VERY_NEGATIVE), axis=1, keepdims=True)
            weight = jnp.where(causal, jnp.exp(line - peak), 0.0)
            scores = lax.dot_general(
                q_ref[rows, cols], k_ref[:upto, cols], (((1,), (1,)), ((), ())),
                preferred_element_type=jnp.float32,
            )
            num[rows, cols] = dot((scores * weight).astype(jnp.bfloat16), v_ref[:upto, cols])
            run[rows, cols] = jnp.broadcast_to(peak, (rows_n, size))

    for peer in range(n_sp):

        @pl.when(peer < sp)
        def _():
            m_copy(peer, peer).wait_recv()
            s_copy(peer, peer).wait_recv()

    def join(j, carried):
        state, start = carried
        stats = srecv[j]
        late_total, late = stats[0:1], stats[1:2]
        joined = jnp.maximum(late_total + start, late)
        state = state * jnp.exp(late_total + start - joined) + mrecv[j].astype(
            jnp.float32
        ) * jnp.exp(late - joined)
        return state, joined

    state, start = lax.fori_loop(
        0, sp, join, (jnp.zeros((size, width), jnp.float32), jnp.zeros((1, width), jnp.float32))
    )
    same = (
        lax.broadcasted_iota(jnp.int32, (width, width), 0) // size
        == lax.broadcasted_iota(jnp.int32, (width, width), 1) // size
    )
    spread = jnp.where(same, jnp.concatenate([state] * heads, axis=0), 0.0).astype(jnp.bfloat16)
    gain = jnp.concatenate([gain_ref[h : h + 1, :] for h in range(heads)], axis=1)
    average = jnp.where(same, 1.0 / size, 0.0)
    for b in range(n_tp):
        rows = slice(b * tokens, (b + 1) * tokens)
        local = run[rows, :]
        peak = jnp.maximum(local, start)
        cell = (
            jnp.exp(local - peak) * num[rows, :] + jnp.exp(start - peak) * dot(q_ref[rows, :], spread)
        ) * size ** (-0.5)
        mean = dot(cell * cell, average, precision=PRECISE)
        normed = cell * lax.rsqrt(mean + EPSILON) * gain
        mixed[b] = (jax.nn.sigmoid(og_ref[rows, :].astype(jnp.float32)) * normed).astype(jnp.bfloat16)

    def a_copy(slot, peer):
        return remote(mixed.at[peer], arecv.at[slot], a_send.at[peer], a_recv.at[slot], {"tp": peer})

    for off in range(1, n_tp):
        a_copy(tp, lax.rem(tp + off, n_tp)).start()
    hooks["exchanged"]()
    weight_copy.wait()

    def part(p):
        return wbuf[pl.ds(pl.multiple_of(p * width, width), width), :]

    acc = dot(mixed[tp], part(tp))
    for off in range(1, n_tp):
        p = lax.rem(tp + off, n_tp)
        a_copy(p, p).wait_recv()
        acc = acc + dot(arecv[p], part(p))
    stream = (res_ref[...].astype(jnp.float32) + acc).astype(jnp.bfloat16)
    stream_ref[...] = stream
    stream = stream.astype(jnp.float32)
    normed_ref[...] = (
        stream * lax.rsqrt(jnp.mean(stream * stream, axis=-1, keepdims=True) + EPSILON) * ngain_ref[...]
    ).astype(jnp.bfloat16)
    for peer in range(1, n_sp):

        @pl.when(peer > sp)
        def _():
            m_copy(sp, peer).wait_send()
            s_copy(sp, peer).wait_send()

    for off in range(1, n_tp):
        a_copy(tp, lax.rem(tp + off, n_tp)).wait_send()


def front(n_sp, n_tp, q, k, v, og, ig_t, fg_t, gain, ow, res, ngain):
    heads = ig_t.shape[0]
    length, width = q.shape
    size = width // heads
    tokens, model = res.shape
    f32, bf16 = jnp.float32, jnp.bfloat16
    dma = pltpu.SemaphoreType.DMA
    return pl.pallas_call(
        functools.partial(front_kernel, n_sp, n_tp, heads, NO_HOOKS),
        out_shape=[jax.ShapeDtypeStruct((tokens, model), bf16)] * 2,
        in_specs=[VMEM] * 7 + [ANY] + [VMEM] * 2,
        out_specs=[VMEM] * 2,
        scratch_shapes=[
            pltpu.VMEM((length, width), f32),
            pltpu.VMEM((length, width), f32),
            pltpu.VMEM((size, width), bf16),
            pltpu.VMEM((8, width), f32),
            pltpu.VMEM((n_sp, size, width), bf16),
            pltpu.VMEM((n_sp, 8, width), f32),
            pltpu.VMEM((n_tp, tokens, width), bf16),
            pltpu.VMEM((n_tp, tokens, width), bf16),
            pltpu.VMEM(ow.shape, bf16),
            dma((n_sp,)), dma((n_sp,)), dma((n_sp,)), dma((n_sp,)), dma((n_tp,)), dma((n_tp,)), dma,
        ],
        compiler_params=pltpu.CompilerParams(
            collective_id=0, has_side_effects=True, vmem_limit_bytes=32 * 2**20
        ),
        cost_estimate=pl.CostEstimate(flops=4 * 10**9, bytes_accessed=8 * 2**20, transcendentals=0),
    )(q, k, v, og, ig_t, fg_t, gain, ow, res, ngain)


def whole_kernel(
    n_sp, n_tp, heads, cap,
    q_ref, k_ref, v_ref, og_ref, ig_ref, fg_ref, gain_ref, ow_ref, res_ref, ngain_ref,
    route_ref, share_ref, score_ref, gate_ref, up_ref, down_ref,
    final_ref,
    q_in, k_in, v_in, og_in, res_in, stream_ref, normed_ref,
    num, run, msend, ssend, mrecv, srecv, mixed, arecv, wbuf,
    gates, ups, downs, buf, tbuf, rows_ref, wts_ref, hidden, kept, xsend, xrecv, zsend, zrecv,
    m_send, m_recv, s_send, s_recv, a_send, a_recv, w_sem,
    in_sem, own_sem, c_send, c_recv, y_send, y_recv, f_send, f_recv,
    z_send, z_recv, x_send, x_recv, wz_send, wz_recv, wx_send, wx_recv,
    bx_send, bx_recv, bz_send, bz_recv,
):
    sp, tp = lax.axis_index("sp"), lax.axis_index("tp")
    z, x = sp // TOP, lax.rem(sp, TOP)
    groups = n_sp // TOP
    tokens = res_ref.shape[0]
    near = {"tp": tp + 1 - 2 * lax.rem(tp, 2)}
    across = {"tp": lax.rem(tp + n_tp // 2, n_tp)}
    other = {"sp": z * TOP + 1 - x}
    depth, model = gate_ref.shape[0], res_ref.shape[1]
    early = depth // 4
    span = model // CHUNKS
    pieces = [
        (gate_ref.at[:early], lambda k: gates.at[k, :early]),
        (gate_ref.at[early:], lambda k: gates.at[k, early:]),
        (up_ref, lambda k: ups.at[k]),
    ] + [
        (down_ref.at[:, c * span : (c + 1) * span], lambda k, c=c: downs.at[k, c])
        for c in range(CHUNKS)
    ]

    pairs = ((k_ref, k_in), (v_ref, v_in), (q_ref, q_in), (og_ref, og_in), (res_ref, res_in))
    loads = [pltpu.make_async_copy(src, dst, in_sem.at[i]) for i, (src, dst) in enumerate(pairs)]
    own, beside, over, onward = [], [], [], []
    for i, (src, at) in enumerate(pieces):
        own.append(pltpu.make_async_copy(src, at(0), own_sem.at[i]))
        beside.append(remote(src, at(1), c_send.at[i], c_recv.at[i], near))
        over.append(remote(src, at(2), y_send.at[i], y_recv.at[i], across))
        onward.append(remote(at(2), at(3), f_send.at[i], f_recv.at[i], near))

    def load():
        for copy in loads:
            copy.start()

    def entered():
        over[0].start()

    def keys():
        loads[0].wait()
        loads[1].wait()

    def queries():
        for copy in loads[2:]:
            copy.wait()
        for copy in beside + own:
            copy.start()

    def exchanged():
        for copy in over[1:]:
            copy.start()

    hooks = {
        "load": load, "entered": entered, "keys": keys, "queries": queries, "exchanged": exchanged,
    }
    front_kernel(
        n_sp, n_tp, heads, hooks,
        q_in, k_in, v_in, og_in, ig_ref, fg_ref, gain_ref, ow_ref, res_in, ngain_ref,
        stream_ref, normed_ref,
        num, run, msend, ssend, mrecv, srecv, mixed, arecv, wbuf,
        m_send, m_recv, s_send, s_recv, a_send, a_recv, w_sem,
    )

    mine = pl.ds(pl.multiple_of(tp * tokens, tokens), tokens)
    first_route = route_ref[:, mine].astype(jnp.float32)[0:1]
    group = jnp.floor(first_route * (1.0 / TOP))
    even = (first_route - TOP * group) < 0.5
    score = score_ref[:, mine]
    power = jnp.exp(score - jnp.max(score, axis=0, keepdims=True))
    route_weight = share_ref[:, mine] * (power / jnp.sum(power, axis=0, keepdims=True))
    lead, rest = route_weight[0:1], route_weight[1:2]
    table = jnp.concatenate(
        [jnp.where(even, lead, rest), jnp.where(even, rest, lead), jnp.zeros((6, tokens), jnp.float32)],
        axis=0,
    )
    hot = lax.broadcasted_iota(jnp.int32, (8, tokens), 0).astype(jnp.float32) == group
    at_row = lax.broadcasted_iota(jnp.int32, (tokens, tokens), 0)
    at_lane = lax.broadcasted_iota(jnp.int32, (tokens, tokens), 1)
    rank = dot(
        jnp.where(hot, 1.0, 0.0).astype(jnp.bfloat16),
        jnp.where(at_row < at_lane, 1.0, 0.0).astype(jnp.bfloat16),
    )
    slot = lax.broadcasted_iota(jnp.int32, (cap, tokens), 0).astype(jnp.float32)
    lane = lax.broadcasted_iota(jnp.int32, (128, tokens), 0).astype(jnp.float32)
    for g in range(groups):
        here = group == float(g)
        pick = jnp.where((slot == rank[g : g + 1]) & here, 1.0, 0.0).astype(jnp.bfloat16)
        wide = jnp.where((lane == rank[g : g + 1]) & here, 1.0, 0.0)
        buf[g] = dot(pick, normed_ref[...]).astype(jnp.bfloat16)
        tbuf[g] = lax.dot_general(
            table, wide, (((1,), (1,)), ((), ())),
            preferred_element_type=jnp.float32, precision=PRECISE,
        )

    def z_copies(slot_z, peer_z):
        to = {"sp": peer_z * TOP + x}
        return (
            remote(tbuf.at[peer_z], wts_ref.at[x, slot_z], wz_send.at[peer_z], wz_recv.at[slot_z], to),
            remote(buf.at[peer_z], rows_ref.at[x, slot_z], z_send.at[peer_z], z_recv.at[slot_z], to),
        )

    def x_own():
        return (
            remote(tbuf.at[z], wts_ref.at[x, z], wx_send.at[z], wx_recv.at[z], other),
            remote(buf.at[z], rows_ref.at[x, z], x_send.at[z], x_recv.at[z], other),
        )

    def x_copies(slot_z, side):
        t, r = wts_ref.at[side, slot_z], rows_ref.at[side, slot_z]
        return (
            remote(t, t, wx_send.at[slot_z], wx_recv.at[slot_z], other),
            remote(r, r, x_send.at[slot_z], x_recv.at[slot_z], other),
        )

    far = [lax.rem(z + off, groups) for off in range(1, groups)]
    for peer in far:
        for copy in z_copies(z, peer):
            copy.start()
    for copy in x_own():
        copy.start()
    rows_ref[x, z] = buf[z]
    wts_ref[x, z] = tbuf[z]
    for copy in own + beside:
        copy.wait()
    over[0].wait()
    onward[0].start()
    for peer in far[::-1]:
        for copy in z_copies(peer, peer):
            copy.wait_recv()
        for copy in x_copies(peer, x):
            copy.start()
    over[1].wait()
    onward[1].start()
    def quarter(k, side):
        block = rows_ref[side].reshape(groups * cap, model)
        hidden[side, k] = (
            jax.nn.silu(dot(block, gates[k])) * dot(block, ups[k])
        ).astype(jnp.bfloat16)

    for k in range(2):
        quarter(k, x)
    for peer in [z] + far[::-1]:
        for copy in x_copies(peer, 1 - x):
            copy.wait_recv()

    def quarters(k):
        @pl.loop(0, 2)
        def _(side):
            quarter(k, side)

    for k in range(2):
        quarter(k, 1 - x)
    over[2].wait()
    onward[2].start()
    quarters(2)
    for i in range(3):
        onward[i].wait()
    quarters(3)

    diagonal = lax.broadcasted_iota(jnp.int32, (cap, cap), 0) == lax.broadcasted_iota(
        jnp.int32, (cap, cap), 1
    )

    def column(side):
        parts = []
        for g in range(groups):
            lines = wts_ref[side, g]
            line = jnp.where(x == 0, lines[0:1, :cap], lines[1:2, :cap])
            parts.append(jnp.sum(jnp.where(diagonal, line, 0.0), axis=1, keepdims=True))
        return jnp.concatenate(parts, axis=0)

    scale_other, scale_own = column(1 - x), column(x)

    def expert(side, c):
        total = dot(hidden[side, 0], downs[0, c])
        for k in range(1, n_tp):
            total = total + dot(hidden[side, k], downs[k, c])
        return total

    def x_copy(c):
        return remote(xsend.at[c], xrecv.at[c], bx_send.at[c], bx_recv.at[c], other)

    def z_copy(c, slot_z, peer_z):
        to = {"sp": peer_z * TOP + x}
        return remote(
            zsend.at[c, peer_z], zrecv.at[c, slot_z], bz_send.at[c, peer_z], bz_recv.at[c, slot_z], to
        )

    def sum_pair(c):
        x_copy(c).wait_recv()
        summed = (kept[c] + xrecv[c].astype(jnp.float32)).astype(jnp.bfloat16)
        zsend[c] = summed.reshape(groups, cap, span)
        for peer in far:
            z_copy(c, z, peer).start()
        zrecv[c, z] = zsend[c, z]

    for c in range(CHUNKS):
        over[3 + c].wait()
        onward[3 + c].start()
        onward[3 + c].wait()
        xsend[c] = (scale_other * expert(1 - x, c)).astype(jnp.bfloat16)
        x_copy(c).start()
        kept[c] = scale_own * expert(x, c)
        if c:
            sum_pair(c - 1)
    sum_pair(CHUNKS - 1)

    def turned(line):
        return jnp.sum(jnp.where(at_row == at_lane, line, 0.0), axis=1, keepdims=True)

    own_rank = turned(jnp.sum(jnp.where(hot, rank, 0.0), axis=0, keepdims=True))
    own_group = turned(group)
    places = lax.broadcasted_iota(jnp.int32, (tokens, groups * cap), 1).astype(jnp.float32)
    pick = jnp.where(places == own_group * cap + own_rank, 1.0, 0.0).astype(jnp.bfloat16)
    for c in range(CHUNKS):
        for peer in far:
            z_copy(c, peer, peer).wait_recv()
        cols = slice(c * span, (c + 1) * span)
        back = dot(pick, zrecv[c].reshape(groups * cap, span))
        final_ref[:, cols] = (stream_ref[:, cols].astype(jnp.float32) + back).astype(jnp.bfloat16)
    for peer in far:
        for copy in z_copies(z, peer):
            copy.wait_send()
        for copy in x_copies(peer, x):
            copy.wait_send()
        for c in range(CHUNKS):
            z_copy(c, z, peer).wait_send()
    for copy in x_own():
        copy.wait_send()
    for c in range(CHUNKS):
        x_copy(c).wait_send()


def whole(
    n_sp, n_tp, cap, q, k, v, og, ig_t, fg_t, gain, ow, res, ngain, route_t, share, score_t,
    gate, up, down,
):
    heads = ig_t.shape[0]
    length, width = q.shape
    size = width // heads
    tokens, model = res.shape
    groups = n_sp // TOP
    f32, bf16 = jnp.float32, jnp.bfloat16
    dma = pltpu.SemaphoreType.DMA
    vm = pltpu.VMEM
    return pl.pallas_call(
        functools.partial(whole_kernel, n_sp, n_tp, heads, cap),
        out_shape=jax.ShapeDtypeStruct((tokens, model), bf16),
        in_specs=[ANY] * 4 + [VMEM] * 3 + [ANY] * 2 + [VMEM] * 4 + [ANY] * 3,
        out_specs=VMEM,
        scratch_shapes=[vm((length, width), bf16)] * 4
        + [vm((tokens, model), bf16)] * 3
        + [
            vm((length, width), f32),
            vm((length, width), f32),
            vm((size, width), bf16),
            vm((8, width), f32),
            vm((n_sp, size, width), bf16),
            vm((n_sp, 8, width), f32),
            vm((n_tp, tokens, width), bf16),
            vm((n_tp, tokens, width), bf16),
            vm(ow.shape, bf16),
            vm((n_tp,) + gate.shape, bf16),
            vm((n_tp,) + up.shape, bf16),
            vm((n_tp, CHUNKS, down.shape[0], model // CHUNKS), bf16),
            vm((groups, cap, model), bf16),
            vm((groups, 8, 128), f32),
            vm((TOP, groups, cap, model), bf16),
            vm((TOP, groups, 8, 128), f32),
            vm((TOP, n_tp, groups * cap, gate.shape[1]), bf16),
            vm((CHUNKS, groups * cap, model // CHUNKS), f32),
        ]
        + [vm((CHUNKS, groups * cap, model // CHUNKS), bf16)] * 2
        + [vm((CHUNKS, groups, cap, model // CHUNKS), bf16)] * 2
        + [dma((n_sp,))] * 4
        + [dma((n_tp,))] * 2
        + [dma, dma((5,))]
        + [dma((3 + CHUNKS,))] * 7
        + [dma((groups,))] * 8
        + [dma((CHUNKS,))] * 2
        + [dma((CHUNKS, groups))] * 2,
        compiler_params=pltpu.CompilerParams(
            collective_id=1, has_side_effects=True, vmem_limit_bytes=60 * 2**20
        ),
    )(q, k, v, og, ig_t, fg_t, gain, ow, res, ngain, route_t, share, score_t, gate, up, down)


def weight_parts(own, axis, count):
    parts = [own]
    for k in range(1, count):
        low = k & -k
        parts.append(lax.ppermute(parts[k ^ low], axis, [(i, i ^ low) for i in range(count)]))
    return parts


def expert_parts(rows, gates, ups, downs):
    total = None
    for gate, up, down in zip(gates, ups, downs):
        hidden = (jax.nn.silu(dot(rows, gate[0])) * dot(rows, up[0])).astype(jnp.bfloat16)
        term = dot(hidden, down[0])
        total = term if total is None else total + term
    return total.astype(jnp.bfloat16)


def slot_within(flat_routes, expert_total):
    onehot = (flat_routes[:, None] == jnp.arange(expert_total, dtype=jnp.int32)[None, :]).astype(
        jnp.int32
    )
    before = jnp.cumsum(onehot, axis=0) - onehot
    return jnp.sum(before * onehot, axis=1)


def fill_slots(source_rows, places, slot_total):
    assign = jnp.arange(places.shape[0], dtype=jnp.int32) // TOP
    owner_index = jnp.full((slot_total,), source_rows.shape[0], jnp.int32).at[places].set(assign)
    padded = jnp.concatenate(
        [source_rows, jnp.zeros((1, source_rows.shape[1]), source_rows.dtype)], axis=0
    )
    return padded[owner_index]


def shards(
    residual, queries, key_vectors, value_vectors, output_gate, input_gate, forget_gate, head_gain,
    output_weight, norm_gain, route_experts, group_weight, expert_scores, gate_weight, up_weight,
    down_weight,
):
    token_count, model_width = residual.shape
    tp = lax.axis_index("tp")
    n_sp, n_tp = lax.axis_size("sp"), lax.axis_size("tp")
    capacity = 2 * TOP * token_count // n_sp
    if n_sp == GROUPS * TOP and n_tp == 4 and token_count == 128:
        return whole(
            n_sp, n_tp, capacity, queries, key_vectors, value_vectors, output_gate, input_gate.T,
            forget_gate.T, head_gain, output_weight, residual,
            norm_gain.reshape(1, -1), route_experts.T, group_weight.reshape(1, -1),
            expert_scores.T, gate_weight[0], up_weight[0], down_weight[0],
        )
    own_routes = lax.dynamic_slice_in_dim(route_experts, tp * token_count, token_count, 0)
    own_group = lax.dynamic_slice_in_dim(group_weight, tp * token_count, token_count, 0)
    own_scores = lax.dynamic_slice_in_dim(expert_scores, tp * token_count, token_count, 0)
    route_weight = own_group[:, None] * jax.nn.softmax(own_scores, axis=-1)
    gates = weight_parts(gate_weight, "tp", n_tp)
    ups = weight_parts(up_weight, "tp", n_tp)
    downs = weight_parts(down_weight, "tp", n_tp)
    stream, normed = front(
        n_sp, n_tp, queries, key_vectors, value_vectors, output_gate, input_gate.T, forget_gate.T,
        head_gain, output_weight, residual, norm_gain.reshape(1, -1),
    )
    flat = own_routes.reshape(-1)
    places = flat * capacity + slot_within(flat, n_sp)
    send_rows = fill_slots(normed, places, n_sp * capacity)
    arrived = lax.all_to_all(
        send_rows.reshape(n_sp, capacity, model_width), "sp", split_axis=0, concat_axis=0, tiled=True
    )
    returned = expert_parts(arrived.reshape(n_sp * capacity, model_width), gates, ups, downs)
    answers = lax.all_to_all(
        returned.reshape(n_sp, capacity, model_width), "sp", split_axis=0, concat_axis=0, tiled=True
    )
    picked = (
        answers.reshape(n_sp * capacity, model_width)[places]
        .astype(jnp.float32)
        .reshape(token_count, TOP, model_width)
    )
    expert_mix = jnp.sum(picked * route_weight[:, :, None], axis=1)
    return (stream.astype(jnp.float32) + expert_mix).astype(jnp.bfloat16)


def solution(mesh):
    return jax.shard_map(
        shards,
        mesh=mesh,
        in_specs=(
            P(("sp", "tp"), None),
            P("sp", "tp"),
            P("sp", "tp"),
            P("sp", "tp"),
            P("sp", "tp"),
            P("sp", "tp"),
            P("sp", "tp"),
            P("tp", None),
            P(),
            P(),
            P("sp", None),
            P("sp"),
            P("sp", None),
            P("sp", None, "tp"),
            P("sp", None, "tp"),
            P("sp", "tp", None),
        ),
        out_specs=P(("sp", "tp"), None),
        check_vma=False,
    )
```
